32 devices in a mesh: ep: 8 (over z, x), tp: 4 (over y, core).
Axes of the slice: x: 2, y: 2, z: 4, core: 2. Of those that a mesh axis runs over, the one named last changes fastest.
Arguments:
- tokens: bfloat16 [64, 2048], P('ep'), may hold values from -6 to 6
- norm_gain: float32 [2048], replicated, may hold values from 0.1 to 1.9
- query_weight: bfloat16 [2048, 1024], P('ep', 'tp'), may hold values from -0.125 to 0.125
- key_weight: bfloat16 [2048, 512], P('ep', 'tp'), may hold values from -0.125 to 0.125
- value_weight: bfloat16 [2048, 512], P('ep', 'tp'), may hold values from -0.125 to 0.125
- query_gain: float32 [64], replicated, may hold values from 0.9 to 1.9
- key_gain: float32 [64], replicated, may hold values from 0.9 to 1.9
- lambdas: float32 [8], P('tp'), may hold values from 0.3 to 0.8
- key_cache: bfloat16 [64, 4, 320, 128], P('ep', 'tp'), may hold values from -5 to 5
- value_cache: bfloat16 [64, 4, 320, 128], P('ep', 'tp'), may hold values from -6 to 6
- lengths: int32 [64], P('ep'), may hold values from 1 to 320
- head_gain: float32 [128], replicated, may hold values from 0.1 to 1.9
- out_weight: bfloat16 [1024, 2048], P('tp', 'ep'), may hold values from -0.1875 to 0.1875
- ffn_gain: float32 [2048], replicated, may hold values from 0.1 to 1.9
- dense_gate_weight: bfloat16 [2048, 1024], P('ep', 'tp'), may hold values from -0.125 to 0.125
- dense_up_weight: bfloat16 [2048, 1024], P('ep', 'tp'), may hold values from -0.125 to 0.125
- dense_down_weight: bfloat16 [1024, 2048], P('tp', 'ep'), may hold values from -0.1875 to 0.1875
- branch_gate: float32 [2048], replicated, may hold values from -0.125 to 0.125
- expert_ids: int32 [64, 2], P('ep'), may hold values from 0 to 15, all different within a row; in each aligned block of 8 rows (0 to 7, 8 to 15, ...) at most 2 rows name the same one
- expert_probs: float32 [64, 2], P('ep'), may hold values from 0.1 to 0.9
- expert_gate: bfloat16 [16, 2048, 5632], P('ep', None, 'tp'), may hold values from -0.125 to 0.125
- expert_up: bfloat16 [16, 2048, 5632], P('ep', None, 'tp'), may hold values from -0.125 to 0.125
- expert_down: bfloat16 [16, 5632, 2048], P('ep', 'tp'), may hold values from -0.078125 to 0.078125
Outputs:
- mixed: bfloat16 [64, 2048], P('ep', 'tp')
The draws below stay inside these ranges and needn't reach their ends.
Inputs may be any that keep to these rules, and one draw needn't show every extreme that they name: `expert_ids`: each row names 2 different experts. Within each aligned block of 8 rows (the sequences of one index of ep) no expert is named more than 2 times, and in every draw some block names some expert exactly 2 times.
All inputs are finite; a program needn't handle non-finite values.
Results may differ from the reference program's by a relative error of at most 0.014.
Values may be sent and summed in bfloat16 or wider, within the bound.
A program may use at most 128 MiB of HBM per device.

```python
import math
import jax
import jax.numpy as jnp
import numpy as np
from jax import lax

D = 2048
HQ = 8
KVH = 4
SUB = 64
VD = 128
FFD = 1024
EXPERTS = 16
FF = 5632
TOP = 2
SEQ_DEV = 8
CACHE = 320
SEQS = 64
REP = 1
SLOTS = 16
CAP = 2
N_EP = 8
N_TP = 4


def set_ends(entries, own_key, low, top_value):
    longest = entries.shape.index(max(entries.shape))
    spots = []
    for shift in (0, 1):
        where = [jax.random.randint(jax.random.fold_in(own_key, axis), (), 0, length) for axis, length in enumerate(entries.shape)]
        where[longest] = (where[longest] + shift) % entries.shape[longest]
        spots.append(tuple(where))
    return entries.at[spots[0]].set(low).at[spots[1]].set(top_value)


def level_of(own_key, shape, split, least, top_value):
    level, own = 1.0, jax.random.fold_in(own_key, 6)
    for axis_at, shards_of in split:
        heights = jnp.exp(jax.random.uniform(jax.random.fold_in(own, axis_at), (shards_of,), jnp.float32, least / len(split), top_value / len(split)))
        level = level * jnp.repeat(heights, shape[axis_at] // shards_of).reshape([-1 if axis == axis_at else 1 for axis in range(len(shape))])
    return level


def routed_block(key, own, number, rows, amount, top, bound, skew):
    sequence = jax.random.permutation(key, amount)
    crowded, usual = load_shares(amount, rows * top, bound, skew, True), load_shares(amount, rows * top, bound, skew, False)
    places = jnp.arange(amount)

    def named(sizes, offset_by):
        used = int((sizes > 0).sum())
        fixed = max(1, used // 4)
        passed = fixed + (places - fixed + offset_by * (used - fixed)) % max(1, amount - fixed)
        return jnp.zeros((amount,), jnp.int32).at[sequence[jnp.where(places < fixed, places, passed)]].set(jnp.asarray(sizes, jnp.int32))

    sizes = jnp.where(number % 4 == 0, named(crowded, number // 4), named(usual, number - number // 4 - 1))
    mixed = jax.random.permutation(jax.random.fold_in(own, 3), amount)
    giver, receiver = mixed[0:amount // 2 * 2:2], mixed[1:amount // 2 * 2:2]
    room = jnp.minimum(sizes[giver] - 1, bound - sizes[receiver]) // 2
    room = jnp.where((giver == sequence[0]) | (receiver == sequence[0]) | (sizes[receiver] == 0), 0, jnp.maximum(room, 0))
    passed = jax.random.randint(jax.random.fold_in(own, 4), (amount // 2,), 0, 1 << 20) % (room + 1)
    sizes = sizes.at[giver].add(-passed).at[receiver].add(passed)
    members = jnp.searchsorted(jnp.cumsum(sizes), jnp.arange(rows * top), side="right").astype(jnp.int32)
    table = members.reshape(top, rows).T
    table = table[jax.random.permutation(jax.random.fold_in(own, 1), rows)]
    offset_by = jax.random.randint(jax.random.fold_in(own, 2), (rows, 1), 0, top)
    return jnp.take_along_axis(table, (jnp.arange(top)[None, :] + offset_by) % top, axis=1)


def load_shares(amount, total, reach, slope, full):
    weights = [(1 << 20) // math.isqrt(rank ** slope) + 1 for rank in range(1, amount + 1)]
    largest = reach if full else min(reach, max(-(-total // amount), total * weights[0] // sum(weights)))
    least = 1 if total - largest >= amount - 1 else 0
    given, surplus = [largest] + [least] * (amount - 1), total - largest - least * (amount - 1)
    while surplus > 0:
        free = [i for i in range(1, amount) if given[i] < largest] or [i for i in range(1, amount) if given[i] < reach]
        mass, budget = sum([weights[i] for i in free]), surplus
        for i in free:
            more = min(reach - given[i], max(1, budget * weights[i] // mass), surplus)
            given[i] = given[i] + more
            surplus = surplus - more
    return np.array(given)


def scatter_about(own_key, shape, deviation, limit, shards=(), kind=jnp.bfloat16):
    values = jax.random.normal(own_key, shape, jnp.float32) * deviation
    if len(shards) > 0:
        values = level_of(own_key, shape, shards, -0.22, 0.18) * values
    return jnp.clip(values, min=-limit, max=limit).astype(kind)


def setup_inputs(seed: int = 0) -> dict:
    splits = jax.random.split(jax.random.key(seed), 24)
    tokens = scatter_about(splits[0], (SEQS, D), 1.0, 6.0, ((0, 8),))
    norm_gain = jnp.clip(1.0 + 0.18 * jax.random.normal(splits[1], (D,), jnp.float32), 0.1, 1.9)
    query_weight = scatter_about(splits[2], (D, 2 * HQ * SUB), D ** -0.5, 0.125, ((0, 8), (1, 4)))
    key_weight = scatter_about(splits[3], (D, 2 * KVH * SUB), D ** -0.5, 0.125, ((0, 8), (1, 4)))
    value_weight = scatter_about(splits[4], (D, KVH * VD), D ** -0.5, 0.125, ((0, 8), (1, 4)))
    query_gain = jnp.clip(jnp.exp(jax.random.uniform(splits[5], (SUB,), jnp.float32, math.log(0.9), math.log(1.9))), 0.9, 1.9)
    key_gain = jnp.clip(jnp.exp(jax.random.uniform(splits[6], (SUB,), jnp.float32, math.log(0.9), math.log(1.9))), 0.9, 1.9)
    lambdas = jnp.clip(0.3 + 0.5 * jax.random.uniform(splits[7], (HQ,), jnp.float32) ** level_of(splits[7], (HQ,), ((0, 4),), -0.2, 0.2), 0.3, 0.8)
    key_cache = scatter_about(splits[8], (SEQS, KVH, CACHE, 2 * SUB), 1.0, 5.0, ((0, 8), (1, 4)))
    value_cache = scatter_about(splits[9], (SEQS, KVH, CACHE, VD), 1.0, 6.0, ((0, 8), (1, 4)))
    lengths = set_ends(jax.random.randint(splits[10], (SEQS,), 1, CACHE + 1), jax.random.fold_in(splits[10], 1), 1, CACHE).astype(jnp.int32)
    head_gain = jnp.clip(1.0 + 0.18 * jax.random.normal(splits[11], (VD,), jnp.float32), 0.1, 1.9)
    out_weight = scatter_about(splits[12], (HQ * VD, D), (HQ * VD) ** -0.5, 0.1875, ((0, 4), (1, 8)))
    ffn_gain = jnp.clip(1.0 + 0.18 * jax.random.normal(splits[13], (D,), jnp.float32), 0.1, 1.9)
    dense_gate_weight = scatter_about(splits[14], (D, FFD), D ** -0.5, 0.125, ((0, 8), (1, 4)))
    dense_up_weight = scatter_about(splits[15], (D, FFD), D ** -0.5, 0.125, ((0, 8), (1, 4)))
    dense_down_weight = scatter_about(splits[16], (FFD, D), FFD ** -0.5, 0.1875, ((0, 4), (1, 8)))
    branch_gate = scatter_about(splits[17], (D,), D ** -0.5, 0.125, (), jnp.float32)
    expert_ids_keys = jax.random.split(jax.random.fold_in(splits[18], 1), SEQS // SEQ_DEV)
    expert_ids_turns = jax.random.permutation(jax.random.fold_in(splits[18], 3), SEQS // SEQ_DEV)
    expert_ids = jax.vmap(lambda own, number: routed_block(jax.random.fold_in(splits[18], 2), own, number, SEQ_DEV, EXPERTS, TOP, CAP, 2))(expert_ids_keys, expert_ids_turns).reshape((SEQS, TOP))
    expert_probs = jnp.clip(0.1 + 0.79999997 * jax.random.uniform(splits[19], (SEQS, TOP), jnp.float32) ** level_of(splits[19], (SEQS, TOP), ((0, 8),), -0.2, 0.2), 0.1, 0.9)
    expert_gate = scatter_about(splits[20], (SLOTS, D, FF // REP), D ** -0.5, 0.125, ((0, 8), (2, 4)))
    expert_up = scatter_about(splits[21], (SLOTS, D, FF // REP), D ** -0.5, 0.125, ((0, 8), (2, 4)))
    expert_down = scatter_about(splits[22], (SLOTS, FF // REP, D), FF ** -0.5, 0.078125, ((0, 8), (1, 4)))
    return {"tokens": tokens, "norm_gain": norm_gain, "query_weight": query_weight, "key_weight": key_weight, "value_weight": value_weight, "query_gain": query_gain, "key_gain": key_gain, "lambdas": lambdas, "key_cache": key_cache, "value_cache": value_cache, "lengths": lengths, "head_gain": head_gain, "out_weight": out_weight, "ffn_gain": ffn_gain, "dense_gate_weight": dense_gate_weight, "dense_up_weight": dense_up_weight, "dense_down_weight": dense_down_weight, "branch_gate": branch_gate, "expert_ids": expert_ids, "expert_probs": expert_probs, "expert_gate": expert_gate, "expert_up": expert_up, "expert_down": expert_down}


epsilon = 1e-06

def rms_scale(values, scaling):
    return values * lax.rsqrt(lax.optimization_barrier(jnp.mean(values * values, axis=-1, keepdims=True)) + epsilon) * scaling

def settle(values):
    return lax.optimization_barrier(values.astype(jnp.bfloat16)).astype(jnp.float32)

def grouped_product(operand, weight, groups):
    seq_count = operand.shape[0]
    depth = operand.shape[1] // groups
    parts = operand.reshape(seq_count, groups, depth)
    blocks = weight.astype(jnp.float32).reshape(groups, depth, weight.shape[1])
    partial_value = settle(jnp.einsum('sgk,gkd->sgd', parts, blocks))
    return lax.optimization_barrier(jnp.sum(partial_value, axis=1))

def block_ranks(expert_ids):
    paired = expert_ids.reshape(N_EP, SEQ_DEV * TOP)
    onehot = (paired[:, :, None] == jnp.arange(EXPERTS, dtype=jnp.int32)[None, None, :]).astype(jnp.int32)
    earlier = (jnp.cumsum(onehot, axis=1) - onehot).astype(jnp.int32)
    return lax.optimization_barrier(jnp.sum(earlier * onehot, axis=2)).astype(jnp.int32).reshape(SEQS, TOP)

def reference(tokens, norm_gain, query_weight, key_weight, value_weight, query_gain, key_gain, lambdas, key_cache, value_cache, lengths, head_gain, out_weight, ffn_gain, dense_gate_weight, dense_up_weight, dense_down_weight, branch_gate, expert_ids, expert_probs, expert_gate, expert_up, expert_down):
    residual = tokens.astype(jnp.float32)
    normed = rms_scale(residual, norm_gain).astype(jnp.bfloat16)
    queries = settle(jnp.dot(normed, query_weight, preferred_element_type=jnp.float32))
    new_keys = settle(jnp.dot(normed, key_weight, preferred_element_type=jnp.float32))
    new_values = settle(jnp.dot(normed, value_weight, preferred_element_type=jnp.float32))
    per_group = HQ // KVH
    score_scale = SUB ** (-0.5)
    lam_heads = lambdas.reshape(1, KVH, per_group)

    def attend_block(inputs):
        block_queries, block_keys, block_values, block_cache, block_store, block_lengths = inputs
        seq_count = block_queries.shape[0]
        query_parts = settle(rms_scale(block_queries.reshape(seq_count, KVH, per_group, 2, SUB), query_gain))
        key_parts = settle(rms_scale(block_keys.reshape(seq_count, KVH, 2, SUB), key_gain))
        cached = settle(rms_scale(block_cache.astype(jnp.float32).reshape(seq_count, KVH, CACHE, 2, SUB), key_gain))
        scores = jnp.einsum('sgqcd,sgjcd->sgqcj', query_parts, cached) * score_scale
        own_score = jnp.einsum('sgqcd,sgcd->sgqc', query_parts, key_parts) * score_scale
        live_mask = jnp.arange(CACHE, dtype=jnp.int32)[None, :] < block_lengths[:, None]
        exponent = jnp.where(live_mask[:, None, None, None, :], jnp.exp(scores), 0.0)
        own_exponent = jnp.exp(own_score)
        denominator = lax.optimization_barrier(jnp.sum(exponent, axis=4)) + own_exponent
        shares = exponent / denominator[..., None]
        own_shares = own_exponent / denominator
        mixing = settle(shares[:, :, :, 0] - lam_heads[..., None] * shares[:, :, :, 1])
        own_mixing = settle(own_shares[:, :, :, 0] - lam_heads * own_shares[:, :, :, 1])
        head_out = jnp.einsum('sgqj,sgje->sgqe', mixing, block_store.astype(jnp.float32))
        head_out = head_out + own_mixing[..., None] * block_values.reshape(seq_count, KVH, VD)[:, :, None, :]
        return settle(rms_scale(head_out, head_gain)).reshape(seq_count, HQ * VD)
    blocks_in = (queries.reshape(N_EP, SEQ_DEV, -1), new_keys.reshape(N_EP, SEQ_DEV, -1), new_values.reshape(N_EP, SEQ_DEV, -1), key_cache.reshape(N_EP, SEQ_DEV, KVH, CACHE, 2 * SUB), value_cache.reshape(N_EP, SEQ_DEV, KVH, CACHE, VD), lengths.reshape(N_EP, SEQ_DEV))
    heads = lax.map(attend_block, blocks_in).reshape(SEQS, HQ * VD)
    attended = grouped_product(heads, out_weight, N_TP)
    middle = settle(residual + attended)
    ffn_input = settle(rms_scale(middle, ffn_gain))
    ffn_rows = ffn_input.astype(jnp.bfloat16)
    dense_gate = jnp.dot(ffn_rows, dense_gate_weight, preferred_element_type=jnp.float32)
    dense_up = jnp.dot(ffn_rows, dense_up_weight, preferred_element_type=jnp.float32)
    dense_hidden = settle(jax.nn.silu(dense_gate) * dense_up)
    dense_out = grouped_product(dense_hidden, dense_down_weight, N_TP)
    branch_weight = jax.nn.sigmoid(lax.optimization_barrier(jnp.sum(ffn_input * branch_gate, axis=1)))
    slot_ranks = block_ranks(expert_ids)
    rows_per = N_EP * CAP
    source = (jnp.arange(SEQS, dtype=jnp.int32) // SEQ_DEV)[:, None]
    slot_index = (expert_ids * rows_per + source * CAP + slot_ranks).astype(jnp.int32)
    slot_rows = jnp.zeros((EXPERTS * rows_per, D), jnp.bfloat16).at[slot_index.reshape(-1)].set(jnp.repeat(ffn_rows, TOP, axis=0))
    slot_rows = slot_rows.reshape(EXPERTS, rows_per, D)
    block_width = FF // REP
    piece_width = FF // (REP * N_TP)
    gate_slots = expert_gate.reshape(REP, EXPERTS, D, block_width)
    up_slots = expert_up.reshape(REP, EXPERTS, D, block_width)
    down_slots = expert_down.reshape(REP, EXPERTS, block_width, D)

    def one_expert(expert_index):
        rows_in = lax.dynamic_index_in_dim(slot_rows, expert_index, 0, False).astype(jnp.float32)
        gate_block = lax.dynamic_index_in_dim(gate_slots, expert_index, 1, False).astype(jnp.float32)
        up_block = lax.dynamic_index_in_dim(up_slots, expert_index, 1, False).astype(jnp.float32)
        down_block = lax.dynamic_index_in_dim(down_slots, expert_index, 1, False).astype(jnp.float32).reshape(REP, N_TP, piece_width, D)
        gate_val = jnp.einsum('rd,bdf->brf', rows_in, gate_block)
        up_val = jnp.einsum('rd,bdf->brf', rows_in, up_block)
        hidden = settle(jax.nn.silu(gate_val) * up_val).reshape(REP, rows_per, N_TP, piece_width)
        partial_value = settle(jnp.einsum('brtf,btfd->brtd', hidden, down_block))
        block_out = settle(lax.optimization_barrier(jnp.sum(partial_value, axis=2)))
        return lax.optimization_barrier(jnp.sum(block_out, axis=0))
    expert_out = lax.map(one_expert, jnp.arange(EXPERTS, dtype=jnp.int32)).reshape(EXPERTS * rows_per, D)
    picked = expert_out[slot_index]
    routed = lax.optimization_barrier(jnp.sum(expert_probs[:, :, None] * picked, axis=1))
    combined = middle + branch_weight[:, None] * dense_out + routed
    return combined.astype(jnp.bfloat16)
```

```python
import functools

import jax
import jax.numpy as jnp
import numpy as np
from jax import lax
from jax.experimental import pallas as pl
from jax.experimental.pallas import tpu as pltpu
from jax.sharding import PartitionSpec as P

SUB = 64
VD = 128
EXPERTS = 16
TOP = 2
CAP = 2


epsilon = 1e-06


def rms_scale(values, scaling):
    return values * lax.rsqrt(jnp.mean(values * values, axis=-1, keepdims=True) + epsilon) * scaling


def project_rows(normed, weights):
    ep_count = lax.axis_size("ep")
    seq_here = normed.shape[0]
    stacked = jnp.concatenate(weights, axis=1)
    columns = lax.all_to_all(normed, "ep", split_axis=1, concat_axis=0, tiled=True)
    partial_value = jnp.dot(columns, stacked, preferred_element_type=jnp.float32).astype(jnp.bfloat16)
    received = lax.all_to_all(partial_value, "ep", split_axis=0, concat_axis=0, tiled=True)
    received = received.reshape(ep_count, seq_here, stacked.shape[1])
    return jnp.sum(received.astype(jnp.float32), axis=0)


def project_back(operand, weight):
    tp_count = lax.axis_size("tp")
    seq_here = operand.shape[0]
    every_row = lax.all_gather(operand, "ep", axis=0, tiled=True)
    partial_value = jnp.dot(every_row, weight, preferred_element_type=jnp.float32).astype(jnp.bfloat16)
    rows = lax.all_to_all(partial_value, "ep", split_axis=0, concat_axis=1, tiled=True)
    pieces = lax.all_to_all(rows, "tp", split_axis=1, concat_axis=0, tiled=True)
    pieces = pieces.reshape(tp_count, seq_here, pieces.shape[1])
    return jnp.sum(pieces.astype(jnp.float32), axis=0)


def attend(packed, key_cache, value_cache, lengths, query_gain, key_gain, lambdas, head_gain):
    seq_here = packed.shape[0]
    kv_here = key_cache.shape[1]
    cache_len = key_cache.shape[2]
    heads_here = lambdas.shape[0]
    per_group = heads_here // kv_here
    query_end = heads_here * 2 * SUB
    key_end = query_end + kv_here * 2 * SUB
    mixed = lax.optimization_barrier(packed.astype(jnp.bfloat16))
    query_parts = rms_scale(
        mixed[:, :query_end].astype(jnp.float32).reshape(seq_here, kv_here, per_group, 2, SUB),
        query_gain,
    ).astype(jnp.bfloat16)
    key_parts = rms_scale(
        mixed[:, query_end:key_end].astype(jnp.float32).reshape(seq_here, kv_here, 2, SUB), key_gain
    ).astype(jnp.bfloat16)
    new_values = mixed[:, key_end:].reshape(seq_here, kv_here, VD)
    cached = rms_scale(
        key_cache.astype(jnp.float32).reshape(seq_here, kv_here, cache_len, 2, SUB), key_gain
    ).astype(jnp.bfloat16)
    score_scale = SUB ** (-0.5)
    scores = (
        jnp.einsum("sgqcd,sgjcd->sgqcj", query_parts, cached, preferred_element_type=jnp.float32)
        * score_scale
    )
    own_score = (
        jnp.einsum("sgqcd,sgcd->sgqc", query_parts, key_parts, preferred_element_type=jnp.float32)
        * score_scale
    )
    live_mask = lax.broadcasted_iota(jnp.int32, (seq_here, cache_len), 1) < lengths[:, None]
    exponent = jnp.where(live_mask[:, None, None, None, :], jnp.exp(scores), 0.0)
    own_exponent = jnp.exp(own_score)
    denominator = jnp.sum(exponent, axis=4) + own_exponent
    shares = exponent / denominator[..., None]
    own_shares = own_exponent / denominator
    lam_heads = lambdas.reshape(1, kv_here, per_group)
    mixing = (shares[:, :, :, 0] - lam_heads[..., None] * shares[:, :, :, 1]).astype(jnp.bfloat16)
    own_mixing = lax.optimization_barrier(
        (own_shares[:, :, :, 0] - lam_heads * own_shares[:, :, :, 1]).astype(jnp.bfloat16)
    )
    head_out = jnp.einsum(
        "sgqj,sgje->sgqe", mixing, value_cache, preferred_element_type=jnp.float32
    )
    head_out = (
        head_out
        + own_mixing.astype(jnp.float32)[..., None] * new_values.astype(jnp.float32)[:, :, None, :]
    )
    return rms_scale(head_out, head_gain).astype(jnp.bfloat16).reshape(seq_here, heads_here * VD)


def route_tables(expert_ids, expert_probs):
    seq_here = expert_ids.shape[0]
    paired = expert_ids.reshape(-1)
    total_pairs = paired.shape[0]
    onehot = (paired[:, None] == lax.broadcasted_iota(jnp.int32, (total_pairs, EXPERTS), 1)).astype(
        jnp.float32
    )
    earlier = (
        lax.broadcasted_iota(jnp.int32, (total_pairs, total_pairs), 1)
        < lax.broadcasted_iota(jnp.int32, (total_pairs, total_pairs), 0)
    ).astype(jnp.float32)
    before = jnp.dot(earlier, onehot, precision=lax.Precision.HIGHEST)
    slot_ranks = jnp.sum(before * onehot, axis=1).astype(jnp.int32)
    slot_codes = (paired * CAP + slot_ranks).reshape(seq_here, TOP)
    slots_iota = lax.broadcasted_iota(jnp.int32, (seq_here, TOP, EXPERTS * CAP), 2)
    picked = (slot_codes[:, :, None] == slots_iota).astype(jnp.float32)
    select = jnp.sum(picked, axis=1)
    combine_weights = jnp.sum(picked * expert_probs[:, :, None], axis=1)
    return (select, combine_weights)


def mixture(ffn_input, expert_ids, expert_probs, expert_gate, expert_up, expert_down):
    here_count = expert_gate.shape[0]
    ep_count = lax.axis_size("ep")
    tp_count = lax.axis_size("tp")
    slot_count = ep_count * here_count
    rep_count = slot_count // EXPERTS
    model_width = ffn_input.shape[1]
    feature_share = model_width // tp_count
    select, combine_weights = route_tables(expert_ids, expert_probs)
    sent_width = ffn_input.shape[1]
    chosen = jnp.einsum(
        "sk,sd->kd", select.astype(jnp.bfloat16), ffn_input, preferred_element_type=jnp.float32
    ).astype(jnp.bfloat16)
    outgoing = jnp.broadcast_to(
        chosen.reshape(1, EXPERTS, CAP, sent_width), (rep_count, EXPERTS, CAP, sent_width)
    ).reshape(slot_count, CAP, sent_width)
    incoming = lax.all_to_all(outgoing, "ep", split_axis=0, concat_axis=0, tiled=True)
    grouped = incoming.reshape(ep_count, here_count, incoming.shape[1], model_width)
    gate_val = jnp.einsum(
        "ihcd,hdf->ihcf", grouped, expert_gate, preferred_element_type=jnp.float32
    )
    up_val = jnp.einsum("ihcd,hdf->ihcf", grouped, expert_up, preferred_element_type=jnp.float32)
    hidden = (jax.nn.silu(gate_val) * up_val).astype(jnp.bfloat16)
    partial_value = jnp.einsum(
        "ihcf,hfd->ihcd", hidden, expert_down, preferred_element_type=jnp.float32
    ).astype(jnp.bfloat16)
    summed = lax.all_to_all(partial_value, "tp", split_axis=3, concat_axis=0, tiled=True)
    block_out = jnp.sum(
        summed.reshape(tp_count, ep_count, here_count, CAP, feature_share).astype(jnp.float32),
        axis=0,
    ).astype(jnp.bfloat16)
    returned = lax.all_to_all(block_out, "ep", split_axis=0, concat_axis=0, tiled=True)
    expert_out = jnp.sum(
        returned.reshape(rep_count, EXPERTS * CAP, feature_share).astype(jnp.float32), axis=0
    )
    return jnp.dot(combine_weights, expert_out, precision=lax.Precision.HIGHEST)


def own_columns(values, tp_start, share_width):
    return lax.dynamic_slice_in_dim(values, tp_start, share_width, 1)


def shards(
    tokens,
    norm_gain,
    query_weight,
    key_weight,
    value_weight,
    query_gain,
    key_gain,
    lambdas,
    key_cache,
    value_cache,
    lengths,
    head_gain,
    out_weight,
    ffn_gain,
    dense_gate_weight,
    dense_up_weight,
    dense_down_weight,
    branch_gate,
    expert_ids,
    expert_probs,
    expert_gate,
    expert_up,
    expert_down,
):
    residual = tokens.astype(jnp.float32)
    normed = rms_scale(residual, norm_gain).astype(jnp.bfloat16)
    packed = project_rows(normed, (query_weight, key_weight, value_weight))
    head_out = attend(
        packed, key_cache, value_cache, lengths, query_gain, key_gain, lambdas, head_gain
    )
    attended = project_back(head_out, out_weight)
    share_width = attended.shape[1]
    tp_start = lax.axis_index("tp") * share_width
    middle_own = (own_columns(residual, tp_start, share_width) + attended).astype(jnp.bfloat16)
    middle = lax.all_gather(middle_own, "tp", axis=1, tiled=True)
    middle_f32 = middle.astype(jnp.float32)
    ffn_input = lax.optimization_barrier(rms_scale(middle_f32, ffn_gain).astype(jnp.bfloat16))
    dense_both = project_rows(ffn_input, (dense_gate_weight, dense_up_weight))
    half_width = dense_both.shape[1] // 2
    hidden = (jax.nn.silu(dense_both[:, :half_width]) * dense_both[:, half_width:]).astype(
        jnp.bfloat16
    )
    dense = project_back(hidden, dense_down_weight)
    branch_weight = jax.nn.sigmoid(
        jnp.sum(ffn_input.astype(jnp.float32) * branch_gate, axis=1, keepdims=True)
    )
    routed = mixture(ffn_input, expert_ids, expert_probs, expert_gate, expert_up, expert_down)
    combined = middle_own.astype(jnp.float32) + branch_weight * dense + routed
    return combined.astype(jnp.bfloat16)


BF = jnp.bfloat16
F32 = jnp.float32
HI = lax.Precision.HIGHEST
MESH = pl.DeviceIdType.MESH


def contract(left, right, dims, precision=None):
    return lax.dot_general(
        left, right, ((dims[0:1], dims[1:2]), ((), ())), precision=precision, preferred_element_type=F32
    )


def silu(values):
    return values / (1.0 + jnp.exp(-values))


def flip(index, bits):
    step = 1
    while step <= bits:
        if bits & step:
            index = index + step - 2 * step * ((index // step) % 2)
        step *= 2
    return index


def split3(values):
    high = values.astype(BF)
    rest = values - high.astype(F32)
    middle = rest.astype(BF)
    low = (rest - middle.astype(F32)).astype(BF)
    return [part.astype(F32) for part in (high, middle, low)]


def in_lanes(columns, rows):
    lane = lax.broadcasted_iota(jnp.int32, (rows, 128), 1)
    out = jnp.zeros((rows, 128), F32)
    for n, column in enumerate(columns):
        out = jnp.where(lane == n, column, out)
    return out


def layer_kernel(
    n_ep, n_tp, tok_hbm, ngain_hbm, wq_hbm, wk_hbm, wv_hbm, qgain_hbm, kgain_hbm, lam_hbm, kc_hbm, vc_hbm,
    len_hbm, hgain_hbm, wo_hbm, fgain_hbm, wdg_hbm, wdu_hbm, wdd_hbm, bgate_hbm, ids_hbm, probs_hbm,
    slot_hbm, eg_hbm, eu_hbm, ed_hbm, out_ref,
    tok_ref, ngain_ref, wq_ref, wk_ref, wv_ref, qgain_ref, kgain_ref, lam_ref, kc_ref, vc_ref,
    len_ref, hgain_ref, wo_ref, fgain_ref, wdg_ref, wdu_ref, wdd_ref, bgate_ref, ids_ref, probs_ref,
    slot_ref, eg, eu, ed, kn, a_send, a_recv, b_send, b_recv, c_send, c_recv, f_send, f_recv, n_send,
    n_recv, m_send, m_recv, i_send, i_recv, j_send, j_recv, g_send, g_recv, disp, acc, unit, sq,
    lsem, wsem, ssem, rsem,
):
    e = lax.axis_index("ep")
    t = lax.axis_index("tp")
    rows, width = tok_ref.shape
    cols = width // n_ep
    seqs = rows * n_ep
    here = eg.shape[0]
    cache_len = kc_ref.shape[0] // rows
    heads = wq_ref.shape[1] // (2 * SUB)
    per_dest = here * CAP
    taken = n_ep * per_dest
    share = width // n_tp
    half = wdg_ref.shape[1]
    per_share = share // cols
    far_ep = sorted(range(1, n_ep), key=lambda k: -(k % 2 + min(k // 2, n_ep // 2 - k // 2)))

    barrier = pltpu.get_barrier_semaphore()
    for k in range(1, n_ep):
        pl.semaphore_signal(barrier, inc=1, device_id={"ep": flip(e, k)}, device_id_type=MESH)
    for k in range(1, n_tp):
        pl.semaphore_signal(barrier, inc=1, device_id={"tp": flip(t, k)}, device_id_type=MESH)

    loads = {}

    def load(name, src, dst):
        copy = pltpu.make_async_copy(src, dst, lsem.at[len(loads)])
        copy.start()
        loads[name] = copy

    def have(*names):
        for name in names:
            loads[name].wait()

    load("tok", tok_hbm, tok_ref)
    load("ids", ids_hbm, ids_ref)
    load("kgain", kgain_hbm, kgain_ref)
    load("kc", kc_hbm, kc_ref)
    load("slot", slot_hbm, slot_ref)
    load("ngain", ngain_hbm, ngain_ref)
    load("wq", wq_hbm, wq_ref)
    load("wk", wk_hbm, wk_ref)
    load("wv", wv_hbm, wv_ref)
    load("wo", wo_hbm, wo_ref.at[t])
    load("len", len_hbm, len_ref)
    load("probs", probs_hbm, probs_ref)
    load("qgain", qgain_hbm, qgain_ref)
    load("lam", lam_hbm, lam_ref)
    load("hgain", hgain_hbm, hgain_ref)
    load("fgain", fgain_hbm, fgain_ref)
    load("bgate", bgate_hbm, bgate_ref)
    load("vc", vc_hbm, vc_ref)
    load("wdg", wdg_hbm, wdg_ref)
    load("wdu", wdu_hbm, wdu_ref)
    load("wdd", wdd_hbm, wdd_ref)

    pending = []
    taken_sems = [0]

    def remote(src, dst, number, device, recv_number=None):
        copy = pltpu.make_async_remote_copy(
            src_ref=src,
            dst_ref=dst,
            send_sem=ssem.at[number],
            recv_sem=rsem.at[number if recv_number is None else recv_number],
            device_id=device,
            device_id_type=MESH,
        )
        return copy

    def numbers(count):
        first = taken_sems[0]
        taken_sems[0] += count
        return first

    def exchange(send, recv, sliced):
        first = numbers(n_ep)
        copies = {}
        for k in far_ep:
            peer = flip(e, k)
            copy = remote(send.at[peer] if sliced else send, recv.at[e], first + k, {"ep": peer})
            copy.start()
            copies[k] = copy
        pending.extend(copies.values())
        recv[e] = send[e] if sliced else send[...]
        return copies

    def arrive(copies):
        for copy in copies.values():
            copy.wait_recv()

    def stack_rows(values):
        return values.astype(F32).reshape(values.shape[0] * values.shape[1], values.shape[2])

    have("tok", "ids")
    tok = tok_ref[...].astype(F32)
    scale = lax.rsqrt(jnp.mean(tok * tok, axis=-1, keepdims=True) + epsilon)
    eye = lax.broadcasted_iota(jnp.int32, (rows, rows), 0) == lax.broadcasted_iota(jnp.int32, (rows, rows), 1)
    lower = lax.broadcasted_iota(jnp.int32, (rows, rows), 1) < lax.broadcasted_iota(jnp.int32, (rows, rows), 0)

    def column(line):
        return jnp.sum(jnp.where(eye, line, 0.0), axis=1, keepdims=True)

    id_lines = [ids_ref[k : k + 1, :].astype(F32) for k in range(TOP)]
    id_columns = [column(line) for line in id_lines]
    codes = []
    for k in range(TOP):
        same = functools.reduce(jnp.logical_or, [id_columns[k] == line for line in id_lines])
        rank = jnp.sum(jnp.where(jnp.logical_and(same, lower), 1.0, 0.0), axis=1, keepdims=True)
        codes.append(id_columns[k] * CAP + rank)
    meta = in_lanes(codes + split3(scale), rows).astype(BF)
    for d in range(n_ep):
        a_send[d, :, :cols] = tok_ref[:, d * cols : (d + 1) * cols]
        a_send[d, :, cols:] = meta

    weight_copies = []
    for n, (src, dst) in enumerate(((eg_hbm, eg), (eu_hbm, eu), (ed_hbm, ed))):
        for h in range(here):
            copy = pltpu.make_async_copy(src.at[h], dst.at[h], wsem.at[h, n])
            copy.start()
            weight_copies.append(copy)

    pl.semaphore_wait(barrier, n_ep - 1 + n_tp - 1)
    a_copies = exchange(a_send, a_recv, True)
    have("wo")
    first = numbers(n_tp)
    wo_copies = {}
    for k in range(1, n_tp):
        copy = remote(wo_ref.at[t], wo_ref.at[t], first + k, {"tp": flip(t, k)})
        copy.start()
        wo_copies[k] = copy
    pending.extend(wo_copies.values())

    lanes = 2 * SUB
    block = (
        (lax.broadcasted_iota(jnp.int32, (lanes, lanes), 0) < SUB)
        == (lax.broadcasted_iota(jnp.int32, (lanes, lanes), 1) < SUB)
    ).astype(F32) * (1.0 / SUB)

    def parts_norm(values, gain):
        mean = jnp.dot(values * values, block, precision=HI, preferred_element_type=F32)
        return (values * lax.rsqrt(mean + epsilon) * gain).astype(BF)

    have("kgain", "kc")
    kgain = jnp.concatenate([kgain_ref[...]] * 2, axis=1)
    for s in range(rows):
        span = slice(s * cache_len, (s + 1) * cache_len)
        kn[span, :] = parts_norm(kc_ref[span, :].astype(F32), kgain)
    have("slot", "ngain", "wq", "wk", "wv")

    arrive(a_copies)
    stacked = stack_rows(a_recv[...])
    tok_cols = stacked[:, :cols]
    meta_all = stacked[:, cols:]
    row_scale = meta_all[:, TOP : TOP + 1] + meta_all[:, TOP + 1 : TOP + 2] + meta_all[:, TOP + 2 : TOP + 3]
    x_cols = (tok_cols * row_scale * ngain_ref[e]).astype(BF)
    start = 0
    for w_ref in (wq_ref, wk_ref, wv_ref):
        stop = start + w_ref.shape[1]
        product = jnp.dot(x_cols, w_ref[...], preferred_element_type=F32)
        b_send[:, :, start:stop] = product.reshape(n_ep, rows, stop - start).astype(BF)
        start = stop
    b_copies = exchange(b_send, b_recv, True)
    slots = slot_ref[...].astype(F32)
    source = (lax.broadcasted_iota(jnp.int32, (seqs, 1), 0) // rows).astype(F32)
    named = functools.reduce(jnp.logical_or, [meta_all[:, k : k + 1] == slots[0:1, :] for k in range(TOP)])
    dispatch = jnp.where(jnp.logical_and(named, source == slots[1:2, :]), 1.0, 0.0).astype(BF)
    unity = (
        lax.broadcasted_iota(jnp.int32, (seqs, seqs), 0) == lax.broadcasted_iota(jnp.int32, (seqs, seqs), 1)
    ).astype(BF)
    disp[...] = contract(dispatch, unity, (0, 0)).astype(BF)
    have("len", "probs", "qgain", "lam", "hgain", "fgain", "bgate", "vc", "wdg", "wdu", "wdd")
    live = lax.broadcasted_iota(jnp.int32, (rows, cache_len), 1).astype(F32) < column(len_ref[...].astype(F32))
    code_lane = lax.broadcasted_iota(jnp.int32, (rows, 128), 1).astype(F32)
    combine = jnp.zeros((rows, 128), F32)
    for k in range(TOP):
        combine = combine + jnp.where(codes[k] == code_lane, column(probs_ref[k : k + 1, :]), 0.0)
    qgain = jnp.concatenate([qgain_ref[...]] * 2, axis=1)
    hgain = hgain_ref[...]
    lam = [lam_ref[:, h : h + 1] for h in range(heads)]

    arrive(b_copies)
    packed = jnp.sum(b_recv[...].astype(F32), axis=0).astype(BF).astype(F32)
    q_end = heads * lanes
    key_part = parts_norm(packed[:, q_end : q_end + lanes], kgain)
    new_value = packed[:, q_end + lanes :]
    low_half = lax.broadcasted_iota(jnp.int32, (rows, lanes), 1) < SUB
    score_scale = SUB ** (-0.5)
    stack, own = [], []
    for h in range(heads):
        query = parts_norm(packed[:, h * lanes : (h + 1) * lanes], qgain).astype(F32)
        own_pair = jnp.dot(
            query * key_part.astype(F32), block, precision=HI, preferred_element_type=F32
        ) * (SUB * score_scale)
        for c in range(2):
            stack.append(jnp.where(low_half if c == 0 else ~low_half, query, 0.0))
            own.append(jnp.exp(own_pair[:, c * SUB : c * SUB + 1]))
    stack = jnp.concatenate(stack, axis=0).astype(BF)
    count = 2 * heads
    row_of = lax.broadcasted_iota(jnp.int32, (count * rows, cache_len), 0) % rows
    scores = jnp.zeros((count * rows, cache_len), F32)
    for s in range(rows):
        product = contract(stack, kn[s * cache_len : (s + 1) * cache_len, :], (1, 1))
        scores = jnp.where(row_of == s, product, scores)
    shares, own_shares = [], []
    for j in range(count):
        exponent = jnp.where(live, jnp.exp(scores[j * rows : (j + 1) * rows] * score_scale), 0.0)
        denominator = jnp.sum(exponent, axis=1, keepdims=True) + own[j]
        shares.append(exponent / denominator)
        own_shares.append(own[j] / denominator)
    mixing = jnp.concatenate(
        [shares[2 * h] - lam[h] * shares[2 * h + 1] for h in range(heads)], axis=0
    ).astype(BF)
    row_out = lax.broadcasted_iota(jnp.int32, (heads * rows, VD), 0) % rows
    mixed_values = jnp.zeros((heads * rows, VD), F32)
    for s in range(rows):
        product = jnp.dot(
            mixing, vc_ref[s * cache_len : (s + 1) * cache_len, :], preferred_element_type=F32
        )
        mixed_values = jnp.where(row_out == s, product, mixed_values)
    for h in range(heads):
        own_mixing = (own_shares[2 * h] - lam[h] * own_shares[2 * h + 1]).astype(BF).astype(F32)
        head_out = mixed_values[h * rows : (h + 1) * rows] + own_mixing * new_value
        c_send[:, h * VD : (h + 1) * VD] = rms_scale(head_out, hgain).astype(BF)
    first = numbers(n_ep * n_tp)
    c_copies = {}
    for k in far_ep + [0]:
        for j in reversed(range(n_tp)):
            if k or j:
                copy = remote(
                    c_send, c_recv.at[t, e], first + k * n_tp + j, {"ep": flip(e, k), "tp": flip(t, j)}
                )
                copy.start()
                c_copies[k, j] = copy
    pending.extend(c_copies.values())
    c_recv[t, e] = c_send[...]
    arrive(wo_copies)
    arrive(c_copies)
    middle = tok_cols
    for c in range(n_tp):
        product = jnp.dot(stack_rows(c_recv[c]).astype(BF), wo_ref[c], preferred_element_type=F32)
        middle = middle + product.astype(BF).astype(F32)
    middle_bf = middle.astype(BF)
    middle = middle_bf.astype(F32)
    moved = jnp.dot(disp[...], middle_bf, preferred_element_type=F32)
    f_send[...] = moved.reshape(n_ep, taken, cols).astype(BF)
    f_copies = exchange(f_send, f_recv, True)
    gained = middle * fgain_ref[e]
    gained_bf = gained.astype(BF)
    n_send[:, :, :half] = (
        jnp.dot(gained_bf, wdg_ref[...], preferred_element_type=F32).reshape(n_ep, rows, half).astype(BF)
    )
    n_send[:, :, half : 2 * half] = (
        jnp.dot(gained_bf, wdu_ref[...], preferred_element_type=F32).reshape(n_ep, rows, half).astype(BF)
    )
    squares = jnp.sum(middle * middle, axis=1, keepdims=True)
    gates = jnp.sum(gained * bgate_ref[e], axis=1, keepdims=True)
    n_send[:, :, 2 * half :] = (
        in_lanes(split3(squares) + split3(gates), seqs).reshape(n_ep, rows, 128).astype(BF)
    )
    n_copies = exchange(n_send, n_recv, True)
    m_send[...] = middle.reshape(n_ep, rows, cols).astype(BF)
    m_first = numbers(n_ep)
    m_slot = lax.rem(e, per_share)
    m_copies = [
        remote(m_send.at[flip(e, k)], m_recv.at[m_slot], m_first + k, {"ep": flip(e, k)}, m_first + m_slot)
        for k in range(1, n_ep)
    ]

    @pl.when(t == e // per_share)
    def _():
        for copy in m_copies:
            copy.start()
        m_recv[m_slot] = m_send[e]

    for copy in weight_copies[: 2 * here]:
        copy.wait()

    def chunk(k):
        d = flip(e, k)
        if k:
            f_copies[k].wait_recv()
        block_rows = pl.ds(pl.multiple_of(d * cols, cols), cols)
        x = f_recv[d].astype(F32)
        part = functools.reduce(
            lambda a, b: a + b, [jnp.square(x[:, i : i + 128]) for i in range(0, cols, 128)]
        )
        operand = (x * fgain_ref[d]).astype(BF)
        for h in range(here):
            for n, ref in enumerate((eg, eu)):
                product = jnp.dot(operand, ref[h, block_rows, :], preferred_element_type=F32)
                if k:
                    acc[h, n] += product
                else:
                    acc[h, n] = product
        if k:
            sq[...] += part
        else:
            sq[...] = part

    near_ep = [0] + far_ep[::-1]
    for k in near_ep[: n_ep - 2]:
        chunk(k)
    arrive(n_copies)
    both = jnp.sum(n_recv[...].astype(F32), axis=0)
    stats = both[:, 2 * half :]
    own_scale = lax.rsqrt(
        (stats[:, 0:1] + stats[:, 1:2] + stats[:, 2:3]) * (1.0 / width) + epsilon
    )
    branch = 1.0 / (1.0 + jnp.exp(-(stats[:, 3:4] + stats[:, 4:5] + stats[:, 5:6]) * own_scale))
    scaled = both[:, : 2 * half] * own_scale
    i_send[...] = (silu(scaled[:, :half]) * scaled[:, half:]).astype(BF)
    i_copies = exchange(i_send, i_recv, False)
    for k in near_ep[n_ep - 2 :]:
        chunk(k)
    r_here = lax.rsqrt(jnp.sum(sq[...], axis=1, keepdims=True) * (1.0 / width) + epsilon)
    owner = (lax.broadcasted_iota(jnp.int32, (taken, 1), 0) % per_dest) // CAP
    for h in range(here):
        kept = owner == h
        unit[h] = jnp.where(kept, silu(acc[h, 0] * r_here) * (acc[h, 1] * r_here), 0.0).astype(BF)
    for copy in weight_copies[2 * here :]:
        copy.wait()
    g_first = numbers(n_ep * n_tp)
    g_copies = {}
    for j in reversed(range(n_tp)):
        c = flip(t, j)
        span = pl.ds(pl.multiple_of(c * share, share), share)
        total = functools.reduce(
            lambda a, b: a + b,
            [jnp.dot(unit[h], ed[h, :, span], preferred_element_type=F32) for h in range(here)],
        )
        for d in range(n_ep):
            g_send[j, d] = total[d * per_dest : (d + 1) * per_dest, :].astype(BF)
        for k in far_ep + [0]:
            if k or j:
                peer = flip(e, k)
                copy = remote(
                    g_send.at[j, peer], g_recv.at[t, e], g_first + j * n_ep + k, {"ep": peer, "tp": c}
                )
                copy.start()
                g_copies[j, k] = copy
    pending.extend(g_copies.values())
    g_recv[t, e] = g_send[0, e]
    arrive(i_copies)
    product = jnp.dot(stack_rows(i_recv[...]).astype(BF), wdd_ref[...], preferred_element_type=F32)
    j_send[...] = product.reshape(n_ep, rows, cols).astype(BF)
    j_tp = e // per_share
    j_first = numbers(max(n_ep, n_tp * per_share))
    j_number = j_first + t * per_share + m_slot
    j_copies = [
        remote(
            j_send.at[flip(e, k)], j_recv.at[t, m_slot], j_first + k, {"ep": flip(e, k), "tp": j_tp}, j_number
        )
        for k in range(n_ep)
    ]
    for copy in j_copies[1:]:
        copy.start()
    pending.extend(j_copies[1:])

    @pl.when(t != j_tp)
    def _():
        j_copies[0].start()

    @pl.when(t == j_tp)
    def _():
        j_recv[t, m_slot] = j_send[e]

    for s in range(per_share):
        copy = remote(m_send.at[0], m_recv.at[s], m_first, {"ep": flip(e, 1)}, m_first + s)

        @pl.when(t * per_share + s != e)
        def _():
            copy.wait_recv()

    result = jnp.concatenate([m_recv[s].astype(F32) for s in range(per_share)], axis=1)
    arrive(g_copies)
    for d in range(n_ep):
        piece = functools.reduce(lambda a, b: a + b, [g_recv[c, d].astype(F32) for c in range(n_tp)])
        piece = piece.astype(BF).astype(F32)
        for i in range(per_dest):
            q = d * per_dest + i
            result = result + combine[:, q : q + 1] * piece[i : i + 1, :]
    for c in range(n_tp):
        for s in range(per_share):
            copy = remote(
                j_send.at[0], j_recv.at[c, s], j_first, {"ep": flip(e, 1)}, j_first + c * per_share + s
            )

            @pl.when(jnp.logical_or(t * per_share + s != e, t != c))
            def _():
                copy.wait_recv()

    dense = functools.reduce(
        lambda a, b: a + b,
        [
            jnp.concatenate([j_recv[c, s].astype(F32) for s in range(per_share)], axis=1)
            for c in range(n_tp)
        ],
    )
    out_ref[...] = (result + branch * dense).astype(BF)
    for copy in pending:
        copy.wait_send()

    @pl.when(t == e // per_share)
    def _():
        for copy in m_copies:
            copy.wait_send()

    @pl.when(t != j_tp)
    def _():
        j_copies[0].wait_send()


def fused_shards(
    tokens, norm_gain, query_weight, key_weight, value_weight, query_gain, key_gain, lambdas, key_cache,
    value_cache, lengths, head_gain, out_weight, ffn_gain, dense_gate_weight, dense_up_weight,
    dense_down_weight, branch_gate, expert_ids, expert_probs, expert_gate, expert_up, expert_down,
):
    n_ep, n_tp = lax.axis_size("ep"), lax.axis_size("tp")
    rows, width = tokens.shape
    cols = width // n_ep
    here, _, hidden_here = expert_gate.shape
    per_dest = here * CAP
    taken = n_ep * per_dest
    share = width // n_tp
    per_share = share // cols
    half = dense_gate_weight.shape[1]
    packed = query_weight.shape[1] + key_weight.shape[1] + value_weight.shape[1]
    seqs = n_ep * rows
    p = np.arange(n_ep * taken)
    slot_table = np.zeros((8, n_ep * taken), np.int32)
    slot_table[0] = (p // taken) * per_dest + p % per_dest
    slot_table[1] = (p // per_dest) % n_ep
    operands = (
        tokens, norm_gain.reshape(n_ep, 1, cols), query_weight, key_weight, value_weight,
        query_gain.reshape(1, SUB), key_gain.reshape(1, SUB), lambdas.reshape(1, -1),
        key_cache.reshape(-1, 2 * SUB), value_cache.reshape(-1, VD), lengths.reshape(1, rows),
        head_gain.reshape(1, VD), out_weight, ffn_gain.reshape(n_ep, 1, cols), dense_gate_weight,
        dense_up_weight, dense_down_weight, branch_gate.reshape(n_ep, 1, cols), expert_ids.T,
        expert_probs.T, jnp.asarray(slot_table), expert_gate, expert_up, expert_down,
    )
    local = [pltpu.VMEM(x.shape, x.dtype) for x in operands]
    local[12] = pltpu.VMEM((n_tp,) + out_weight.shape, BF)
    vmem = pl.BlockSpec(memory_space=pltpu.VMEM)
    hbm = pl.BlockSpec(memory_space=pl.ANY)
    pair = lambda shape: [pltpu.VMEM(shape, BF), pltpu.VMEM(shape, BF)]
    spread = lambda n, shape: [pltpu.VMEM(shape, BF), pltpu.VMEM(n + shape, BF)]
    count = 6 * n_ep + 2 * n_ep * n_tp + n_tp + max(n_ep, n_tp * per_share)
    scratch = [
        *local,
        pltpu.VMEM((rows * key_cache.shape[2], 2 * SUB), BF),
        *pair((n_ep, rows, cols + 128)),
        *pair((n_ep, rows, packed)),
        *spread((n_tp, n_ep), (rows, out_weight.shape[0])),
        *pair((n_ep, taken, cols)),
        *pair((n_ep, rows, 2 * half + 128)),
        pltpu.VMEM((n_ep, rows, cols), BF),
        pltpu.VMEM((per_share, rows, cols), BF),
        *spread((n_ep,), (rows, half)),
        pltpu.VMEM((n_ep, rows, cols), BF),
        pltpu.VMEM((n_tp, per_share, rows, cols), BF),
        *pair((n_tp, n_ep, per_dest, share)),
        pltpu.VMEM((n_ep * taken, seqs), BF),
        pltpu.VMEM((here, 2, taken, hidden_here), F32),
        pltpu.VMEM((here, taken, hidden_here), BF),
        pltpu.VMEM((taken, 128), F32),
        pltpu.SemaphoreType.DMA((24,)),
        pltpu.SemaphoreType.DMA((here, 3)),
        pltpu.SemaphoreType.DMA((count,)),
        pltpu.SemaphoreType.DMA((count,)),
    ]
    return pl.pallas_call(
        functools.partial(layer_kernel, n_ep, n_tp),
        out_shape=jax.ShapeDtypeStruct((rows, share), BF),
        in_specs=[hbm] * len(operands),
        out_specs=vmem,
        scratch_shapes=scratch,
        compiler_params=pltpu.CompilerParams(
            collective_id=0, has_side_effects=True, vmem_limit_bytes=62 * 1024 * 1024
        ),
    )(*operands)


def dispatch_shards(*args):
    tokens, key_cache, expert_gate = args[0], args[8], args[20]
    n_ep, n_tp = lax.axis_size("ep"), lax.axis_size("tp")
    width = tokens.shape[1]
    slots = n_ep * expert_gate.shape[0]
    resident = 3 * expert_gate.size * expert_gate.dtype.itemsize
    fits = (
        slots == EXPERTS
        and n_ep & (n_ep - 1) == 0
        and n_tp & (n_tp - 1) == 0
        and n_ep > 2
        and key_cache.shape[1] == 1
        and tokens.shape[0] == 8
        and width % (128 * n_ep) == 0
        and (width // n_tp) % (width // n_ep) == 0
        and resident <= 40 * 1024 * 1024
    )
    return fused_shards(*args) if fits else shards(*args)


def solution(mesh):
    return jax.shard_map(
        dispatch_shards,
        mesh=mesh,
        in_specs=(
            P("ep", None),
            P(),
            P("ep", "tp"),
            P("ep", "tp"),
            P("ep", "tp"),
            P(),
            P(),
            P("tp"),
            P("ep", "tp", None, None),
            P("ep", "tp", None, None),
            P("ep"),
            P(),
            P("tp", "ep"),
            P(),
            P("ep", "tp"),
            P("ep", "tp"),
            P("tp", "ep"),
            P(),
            P("ep", None),
            P("ep", None),
            P("ep", None, "tp"),
            P("ep", None, "tp"),
            P("ep", "tp", None),
        ),
        out_specs=P("ep", "tp"),
        check_vma=False,
    )
```
